32 devices in a mesh: sp: 8 (over z, y), tp: 4 (over x, core).
Axes of the slice: x: 2, y: 2, z: 4, core: 2. Of those that a mesh axis runs over, the one named last changes fastest.
Arguments:
- grad_out: bfloat16 [2048, 2048], P('sp'), may hold values from -6 to 6
- resid: bfloat16 [2048, 2048], P('sp'), may hold values from -6 to 6
- norm_gain: float32 [2048], replicated, may hold values from 0.1 to 1.9
- routes: int32 [2048, 2], P('sp'), may hold values from 0 to 7, all different within a row; in each aligned block of 256 rows (0 to 255, 256 to 511, ...) at most 96 rows name the same one
- route_weights: float32 [2048, 2], P('sp'), may hold values from 0.05 to 1
- gate_weight: bfloat16 [8, 2048, 1536], P('sp', None, 'tp'), may hold values from -0.375 to 0.375
- up_weight: bfloat16 [8, 2048, 1536], P('sp', None, 'tp'), may hold values from -0.375 to 0.375
- down_weight: bfloat16 [8, 1536, 2048], P('sp', 'tp'), may hold values from -0.15625 to 0.15625
- proj_weight: bfloat16 [2048, 512], P(None, 'tp'), may hold values from -0.25 to 0.25
- conv_sum: bfloat16 [2048, 512], P('sp', 'tp'), may hold values from -6 to 6
- conv_gain: float32 [512], P('tp'), may hold values from 0.1 to 1.9
- conv_taps: float32 [31, 512], P(None, 'tp'), may hold values from -1 to 1
- conv_value: bfloat16 [2048, 512], P('sp', 'tp'), may hold values from -6 to 6
- conv_gate: bfloat16 [2048, 512], P('sp', 'tp'), may hold values from -6 to 6
Outputs:
- gate_weight_grad: bfloat16 [8, 2048, 1536], P('sp', None, 'tp')
- up_weight_grad: bfloat16 [8, 2048, 1536], P('sp', None, 'tp')
- down_weight_grad: bfloat16 [8, 1536, 2048], P('sp', 'tp')
- proj_grad: float32 [2048, 512], P('sp', 'tp')
- value_grad: bfloat16 [2048, 512], P('sp', 'tp')
- gate_input_grad: bfloat16 [2048, 512], P('sp', 'tp')
The draws below stay inside these ranges and needn't reach their ends.
Inputs may be any that keep to these rules, and one draw needn't show every extreme that they name: In each aligned block of 256 tokens no expert is named by more than 96 routes, and in some block one expert is named exactly 96 times; a token's two routes name different experts.
All inputs are finite; a program needn't handle non-finite values.
Results may differ from the reference program's by a relative error of at most 0.028.
Values may be sent and summed in bfloat16 or wider, within the bound.
No kernel may reach another device: no remote copies, remote signals or barrier semaphores. Data moves between devices by JAX's collectives and lax.ppermute only.
A program may use at most 128 MiB of HBM per device.

```python
import math
import jax
import jax.numpy as jnp
import numpy as np
from jax import lax

D = 2048
F = 1536
CH = 512
CONV_K = 31
TOK_DEV = 256
GROUP = 128
EXPERTS = 8
CAP = 96
TOKENS = 2048
N_SP = 8
N_TP = 4


def raised(result, rng, source, target, blocks, factor):
    owner, partner = [(jnp.arange(result.shape[axis_at]) // (result.shape[axis_at] // blocks)).reshape([-1 if axis == axis_at else 1 for axis in range(result.ndim)]) for axis_at in (source, target)]
    chosen = jax.random.permutation(rng, blocks)[partner]
    strong = (owner == chosen) | (owner == (partner + blocks // 2) % blocks)
    return jnp.where(strong, factor * result, result)


def block_levels(key, extent, pieces, smallest, high):
    loudness = 1.0
    for dim, parts in pieces:
        heights = jax.random.uniform(jax.random.fold_in(jax.random.fold_in(key, 6), dim), (parts,), jnp.float32, smallest / len(pieces), high / len(pieces))
        loudness = loudness * jnp.repeat(jnp.exp(heights), extent[dim] // parts).reshape((-1,) + (1,) * (len(extent) - 1 - dim))
    return loudness


def deal_out(own_key, own, number, rows, number_of, top, reach, skew):
    order = jax.random.permutation(own_key, number_of)
    crowded, ordinary = shares(number_of, rows * top, reach, skew, True), shares(number_of, rows * top, reach, skew, False)
    places = jnp.arange(number_of)

    def named(lengths, rotation):
        used = int((lengths > 0).sum())
        fixed = max(1, used // 4)
        passed = fixed + (places - fixed + rotation * (used - fixed)) % max(1, number_of - fixed)
        return jnp.zeros((number_of,), jnp.int32).at[order[jnp.where(places < fixed, places, passed)]].set(jnp.asarray(lengths, jnp.int32))

    lengths = jnp.where(number % 4 == 0, named(crowded, number // 4), named(ordinary, number - number // 4 - 1))
    mixed = jax.random.permutation(jax.random.fold_in(own, 3), number_of)
    giver, receiver = mixed[0:number_of // 2 * 2:2], mixed[1:number_of // 2 * 2:2]
    room = jnp.minimum(lengths[giver] - 1, reach - lengths[receiver]) // 2
    room = jnp.where((giver == order[0]) | (receiver == order[0]) | (lengths[receiver] == 0), 0, jnp.maximum(room, 0))
    passed = jax.random.randint(jax.random.fold_in(own, 4), (number_of // 2,), 0, 1 << 20) % (room + 1)
    lengths = lengths.at[giver].add(-passed).at[receiver].add(passed)
    items = jnp.searchsorted(jnp.cumsum(lengths), jnp.arange(rows * top), side="right").astype(jnp.int32)
    grid = items.reshape(top, rows).T
    grid = grid[jax.random.permutation(jax.random.fold_in(own, 1), rows)]
    rotation = jax.random.randint(jax.random.fold_in(own, 2), (rows, 1), 0, top)
    return jnp.take_along_axis(grid, (jnp.arange(top)[None, :] + rotation) % top, axis=1)


def shares(amount, total, limit, lean, full):
    portions = [(1 << 20) // math.isqrt(standing ** lean) + 1 for standing in range(1, amount + 1)]
    largest = limit if full else min(limit, max(-(-total // amount), total * portions[0] // sum(portions)))
    least = 1 if total - largest >= amount - 1 else 0
    holding, spare = [largest] + [least] * (amount - 1), total - largest - least * (amount - 1)
    while spare > 0:
        candidates = [i for i in range(1, amount) if holding[i] < largest] or [i for i in range(1, amount) if holding[i] < limit]
        pool, remaining = sum([portions[i] for i in candidates]), spare
        for i in candidates:
            addition = min(limit - holding[i], max(1, remaining * portions[i] // pool), spare)
            holding[i] = holding[i] + addition
            spare = spare - addition
    return np.array(holding)


def gaussian(key, extent, deviation, bound, shards=(), held_as=jnp.bfloat16):
    values = deviation * jax.random.normal(key, extent, jnp.float32)
    if shards:
        values = values * block_levels(key, extent, shards, -0.22, 0.18)
    return jnp.clip(values, -bound, bound).astype(held_as)


def noise_with(rng, dims, deviation, limit, split, heavy, kind=jnp.bfloat16):
    drawn = deviation * jax.random.normal(rng, dims, jnp.float32)
    if split:
        drawn = drawn * block_levels(rng, dims, split, -0.22, 0.18)
    return jnp.clip(raised(drawn, jax.random.fold_in(rng, 3), *heavy), -limit, limit).astype(kind)


def setup_inputs(seed: int = 0) -> dict:
    streams_of = jax.random.split(jax.random.key(seed), 15)
    grad_out = noise_with(streams_of[0], (TOKENS, D), 1.0, 6.0, ((0, 8),), (0, 1, 8, 2.0))
    resid = gaussian(streams_of[1], (TOKENS, D), 1.0, 6.0, ((0, 8),))
    norm_gain = jnp.clip(1.0 + 0.18 * jax.random.normal(streams_of[2], (D,), jnp.float32), 0.1, 1.9)
    routes_keys = jax.random.split(jax.random.fold_in(streams_of[3], 1), TOKENS // TOK_DEV)
    routes_turns = jax.random.permutation(jax.random.fold_in(streams_of[3], 3), TOKENS // TOK_DEV)
    routes = jax.vmap(lambda own, number: deal_out(jax.random.fold_in(streams_of[3], 2), own, number, TOK_DEV, EXPERTS, 2, CAP, 1))(routes_keys, routes_turns).reshape((TOKENS, 2))
    route_weights = jnp.clip(0.05 + 0.95 * jax.random.uniform(streams_of[4], (TOKENS, 2), jnp.float32) ** block_levels(streams_of[4], (TOKENS, 2), ((0, 8),), -0.2, 0.2), 0.05, 1.0)
    gate_weight = gaussian(streams_of[5], (EXPERTS, D, F), (D // 9) ** -0.5, 0.375, ((0, 8), (2, 4)))
    up_weight = gaussian(streams_of[6], (EXPERTS, D, F), (D // 9) ** -0.5, 0.375, ((0, 8), (2, 4)))
    down_weight = gaussian(streams_of[7], (EXPERTS, F, D), F ** -0.5, 0.15625, ((0, 8), (1, 4)))
    proj_weight = gaussian(streams_of[8], (D, CH), CH ** -0.5, 0.25, ((1, 4),))
    conv_sum = gaussian(streams_of[9], (TOKENS, CH), 1.0, 6.0, ((0, 8), (1, 4)))
    conv_gain = jnp.clip(1.0 + 0.18 * jax.random.normal(streams_of[10], (CH,), jnp.float32), 0.1, 1.9)
    conv_taps = gaussian(streams_of[11], (CONV_K, CH), CONV_K ** -0.5, 1.0, ((1, 4),), jnp.float32)
    conv_value = gaussian(streams_of[12], (TOKENS, CH), 1.0, 6.0, ((0, 8), (1, 4)))
    conv_gate = gaussian(streams_of[13], (TOKENS, CH), 1.0, 6.0, ((0, 8), (1, 4)))
    return dict(grad_out=grad_out, resid=resid, norm_gain=norm_gain, routes=routes, route_weights=route_weights, gate_weight=gate_weight, up_weight=up_weight, down_weight=down_weight, proj_weight=proj_weight, conv_sum=conv_sum, conv_gain=conv_gain, conv_taps=conv_taps, conv_value=conv_value, conv_gate=conv_gate)


CLAMP_LIMIT = 7.0
SLOPE_ALPHA = 1.702

def contract_rows(left_side, right_side):
    return lax.dot_general(left_side, right_side, (((0,), (0,)), ((), ())), preferred_element_type=jnp.float32)

def contract_cols(left_side, right_side):
    return lax.dot_general(left_side, right_side, (((1,), (1,)), ((), ())), preferred_element_type=jnp.float32)

def expert_backward(routed_rows, routed_cots, w_gate, w_up, w_down):
    gate_pre = jnp.dot(routed_rows, w_gate, preferred_element_type=jnp.float32)
    up_pre = jnp.dot(routed_rows, w_up, preferred_element_type=jnp.float32)
    gate_clamped = jnp.minimum(gate_pre, CLAMP_LIMIT)
    up_clamped = jnp.clip(up_pre, -CLAMP_LIMIT, CLAMP_LIMIT)
    sigma = jax.nn.sigmoid(SLOPE_ALPHA * gate_clamped)
    gated = gate_clamped * sigma
    act = ((up_clamped + 1.0) * gated).astype(jnp.bfloat16)
    down_grad = contract_rows(act, routed_cots).astype(jnp.bfloat16)
    act_grad = contract_cols(routed_cots, w_down)
    inside = (up_pre > -CLAMP_LIMIT) & (up_pre < CLAMP_LIMIT)
    up_pre_grad = jnp.where(inside, act_grad * gated, 0.0).astype(jnp.bfloat16)
    slope = sigma + SLOPE_ALPHA * gate_clamped * sigma * (1.0 - sigma)
    gate_pre_grad = jnp.where(gate_pre < CLAMP_LIMIT, act_grad * (up_clamped + 1.0) * slope, 0.0).astype(jnp.bfloat16)
    gate_grad = contract_rows(routed_rows, gate_pre_grad).astype(jnp.bfloat16)
    up_grad = contract_rows(routed_rows, up_pre_grad).astype(jnp.bfloat16)
    partial_value = contract_cols(gate_pre_grad, w_gate) + contract_cols(up_pre_grad, w_up)
    return (gate_grad, up_grad, down_grad, partial_value)

def reference(grad_out, resid, norm_gain, routes, route_weights, gate_weight, up_weight, down_weight, proj_weight, conv_sum, conv_gain, conv_taps, conv_value, conv_gate):
    resid_f = resid.astype(jnp.float32)
    inv_rms = lax.rsqrt(lax.optimization_barrier(jnp.mean(resid_f * resid_f, axis=-1, keepdims=True)) + 1e-06)
    normed = (resid_f * inv_rms * norm_gain).astype(jnp.bfloat16)
    scaled = (route_weights[:, :, None] * grad_out.astype(jnp.float32)[:, None, :]).astype(jnp.bfloat16)
    scaled = scaled.reshape(2 * TOKENS, D)
    route_ids = routes.reshape(N_SP, 2 * TOK_DEV)
    one_hot = (route_ids[:, :, None] == jnp.arange(EXPERTS, dtype=jnp.int32)[None, None, :]).astype(jnp.int32)
    slot_rank = lax.optimization_barrier(jnp.sum(jnp.cumsum(one_hot, axis=1) * one_hot, axis=2)) - 1
    slot_index = route_ids * (N_SP * CAP) + jnp.arange(N_SP, dtype=jnp.int32)[:, None] * CAP + slot_rank
    slot_table = jnp.full((EXPERTS * N_SP * CAP,), 2 * TOKENS, jnp.int32)
    slot_table = slot_table.at[slot_index.reshape(-1)].set(jnp.arange(2 * TOKENS, dtype=jnp.int32))
    slot_table = slot_table.reshape(EXPERTS, N_SP * CAP)
    normed_pad = jnp.concatenate([normed, jnp.zeros((1, D), jnp.bfloat16)], axis=0)
    scaled_pad = jnp.concatenate([scaled, jnp.zeros((1, D), jnp.bfloat16)], axis=0)
    block_width = F // N_TP

    def one_expert(route_store, inputs):
        table_row, w_gate, w_up, w_down = inputs
        routed_rows = normed_pad[table_row // 2]
        routed_cots = scaled_pad[table_row]
        gate_parts, up_parts, down_parts = ([], [], [])
        row_total = jnp.zeros((N_SP * CAP, D), jnp.float32)
        for block_number in range(N_TP):
            first_col = block_number * block_width
            gate_grad, up_grad, down_grad, partial_value = expert_backward(routed_rows, routed_cots, w_gate[:, first_col:first_col + block_width], w_up[:, first_col:first_col + block_width], w_down[first_col:first_col + block_width, :])
            gate_parts.append(gate_grad)
            up_parts.append(up_grad)
            down_parts.append(down_grad)
            rounded = lax.optimization_barrier(partial_value.astype(jnp.bfloat16))
            row_total = row_total + rounded.astype(jnp.float32)
        route_store = route_store.at[table_row].set(row_total.astype(jnp.bfloat16))
        return (route_store, (jnp.concatenate(gate_parts, axis=1), jnp.concatenate(up_parts, axis=1), jnp.concatenate(down_parts, axis=0)))
    route_store = jnp.zeros((2 * TOKENS + 1, D), jnp.bfloat16)
    route_store, (gate_weight_grad, up_weight_grad, down_weight_grad) = lax.scan(one_expert, route_store, (slot_table, gate_weight, up_weight, down_weight))
    normed_grad = route_store[:2 * TOKENS].astype(jnp.float32).reshape(TOKENS, 2, D).sum(axis=1).astype(jnp.bfloat16)
    feature_grad = normed_grad.astype(jnp.float32) * norm_gain
    cubed = inv_rms * inv_rms * inv_rms
    resid_grad = (grad_out.astype(jnp.float32) + inv_rms * feature_grad - resid_f * cubed * lax.optimization_barrier(jnp.mean(resid_f * feature_grad, axis=-1, keepdims=True))).astype(jnp.bfloat16)
    summed = conv_sum.astype(jnp.float32).reshape(TOKENS, CH // GROUP, GROUP)
    centre = summed - lax.optimization_barrier(jnp.mean(summed, axis=-1, keepdims=True))
    inv_std = lax.rsqrt(lax.optimization_barrier(jnp.mean(centre * centre, axis=-1, keepdims=True)) + 1e-05)
    grouped = centre * inv_std
    chan_normed = grouped.reshape(TOKENS, CH)
    pre_act = chan_normed * conv_gain
    sigma_conv = jax.nn.sigmoid(pre_act)
    conv_out = (pre_act * sigma_conv).astype(jnp.bfloat16)
    proj_grad = contract_rows(resid_grad, conv_out)
    out_grad = jnp.dot(resid_grad, proj_weight, preferred_element_type=jnp.float32)
    normal_grad = (out_grad * sigma_conv * (1.0 + pre_act * (1.0 - sigma_conv)) * conv_gain).reshape(TOKENS, CH // GROUP, GROUP)
    sum_grad = inv_std * (normal_grad - lax.optimization_barrier(jnp.mean(normal_grad, axis=-1, keepdims=True)) - grouped * lax.optimization_barrier(jnp.mean(normal_grad * grouped, axis=-1, keepdims=True)))
    sum_grad = sum_grad.reshape(TOKENS, CH)
    extended = jnp.concatenate([sum_grad, jnp.zeros((CONV_K - 1, CH), jnp.float32)], axis=0)
    gated_grad = lax.conv_general_dilated(extended[None], conv_taps[::-1][:, None, :], (1,), ((0, 0),), dimension_numbers=('NWC', 'WIO', 'NWC'), feature_group_count=CH, precision=lax.Precision.HIGHEST)[0]
    sigma_gate = jax.nn.sigmoid(conv_gate.astype(jnp.float32))
    value_grad = (gated_grad * sigma_gate).astype(jnp.bfloat16)
    gate_input_grad = (gated_grad * conv_value.astype(jnp.float32) * sigma_gate * (1.0 - sigma_gate)).astype(jnp.bfloat16)
    return (gate_weight_grad, up_weight_grad, down_weight_grad, proj_grad, value_grad, gate_input_grad)
```

```python
import jax
import jax.numpy as jnp
from jax import lax
from jax.sharding import PartitionSpec as P

CONV_K = 31
GROUP = 128


CLAMP_LIMIT = 7.0
SLOPE_ALPHA = 1.702
SEND_CHUNKS = 2


def passed_along(block, axis, distance):
    devices = range(lax.axis_size(axis))
    route = [(i - distance, i) for i in devices if i - distance in devices]
    return lax.ppermute(block, axis, route)


def contract_rows(left_side, right_side):
    return lax.dot_general(
        left_side, right_side, (((0,), (0,)), ((), ())), preferred_element_type=jnp.float32
    )


def contract_cols(left_side, right_side):
    return lax.dot_general(
        left_side, right_side, (((1,), (1,)), ((), ())), preferred_element_type=jnp.float32
    )


def exchanged(block, axis, flip):
    route = [(i, i ^ flip) for i in range(lax.axis_size(axis))]
    return lax.ppermute(block, axis, route)


def swapped(blocks):
    return lax.all_to_all(blocks, "sp", split_axis=0, concat_axis=0, tiled=True)


def gather_cols(part, own, count):
    rows, width = part.shape
    parts = {0: part}
    bit = count >> 1
    while bit:
        for flip in sorted(parts):
            parts[flip | bit] = exchanged(parts[flip], "tp", bit)
        bit >>= 1
    full = jnp.zeros((rows, width * count), part.dtype)
    for flip in range(count):
        full = lax.dynamic_update_slice(full, parts[flip], (0, (own ^ flip) * width))
    return full


def scatter_cols(partial, own, count):
    width = partial.shape[1] // count
    parts = {
        flip: lax.dynamic_slice_in_dim(partial, (own ^ flip) * width, width, 1)
        for flip in range(count)
    }
    bit = 1
    while bit < count:
        sent = {}
        for flip in sorted(parts)[::-1]:
            if flip & bit:
                sent[flip] = exchanged(parts[flip], "tp", bit)
        parts = {
            flip: (
                parts[flip].astype(jnp.float32) + sent[flip | bit].astype(jnp.float32)
            ).astype(jnp.bfloat16)
            for flip in parts
            if not flip & bit
        }
        bit <<= 1
    return parts[0]


def backward(
    grad_out,
    resid,
    norm_gain,
    routes,
    route_weights,
    gate_weight,
    up_weight,
    down_weight,
    proj_weight,
    conv_sum,
    conv_gain,
    conv_taps,
    conv_value,
    conv_gate,
):
    tok_rows, model_width = resid.shape
    sp_count = lax.axis_size("sp")
    tp_count = lax.axis_size("tp")
    tp_own = lax.axis_index("tp")
    capacity = 3 * tok_rows // sp_count
    col_count = model_width // tp_count
    send_chunks = SEND_CHUNKS if capacity % (16 * SEND_CHUNKS) == 0 else 1
    piece = capacity // send_chunks
    first_col = tp_own * col_count
    w_gate, w_up, w_down = gate_weight[0], up_weight[0], down_weight[0]

    order = jnp.arange(sp_count, dtype=jnp.int32)
    named = routes.T[:, None, :] == order[None, :, None]
    member = named[0] | named[1]
    earlier = (
        jnp.arange(tok_rows, dtype=jnp.int32)[:, None] < jnp.arange(tok_rows, dtype=jnp.int32)[None, :]
    )
    rank = jnp.dot(
        member.astype(jnp.bfloat16), earlier.astype(jnp.bfloat16), preferred_element_type=jnp.float32
    ).astype(jnp.int32)
    rank = jnp.where(member, rank, -1)
    token_weight = jnp.sum(jnp.where(named, route_weights.T[:, None, :], 0.0), axis=0)
    hit = rank[:, None, :] == jnp.arange(capacity, dtype=jnp.int32)[None, :, None]
    chosen = hit.astype(jnp.bfloat16)
    slot_weight = jnp.sum(jnp.where(hit, token_weight[:, None, :], 0.0), axis=-1)

    resid_f = resid.astype(jnp.float32)
    inv_rms = lax.rsqrt(jnp.mean(resid_f * resid_f, axis=-1, keepdims=True) + 1e-06)
    resid_part = lax.dynamic_slice_in_dim(resid, first_col, col_count, 1).astype(jnp.float32)
    gain_part = lax.dynamic_slice_in_dim(norm_gain, first_col, col_count, 0)
    normed_part = (resid_part * inv_rms * gain_part).astype(jnp.bfloat16)
    cots_part = lax.dynamic_slice_in_dim(grad_out, first_col, col_count, 1)

    select = chosen.reshape(sp_count * capacity, tok_rows)

    def sent_out(value):
        return swapped(value.reshape(sp_count, -1, col_count))

    def pieces(value):
        return [
            value[:, chunk * piece : (chunk + 1) * piece].reshape(-1, col_count)
            for chunk in range(send_chunks)
        ]

    rows_out = jnp.dot(select, normed_part, preferred_element_type=jnp.float32)
    cots_out = jnp.dot(select, cots_part, preferred_element_type=jnp.float32)
    cots_out = cots_out * slot_weight.reshape(-1, 1)
    rows_in = pieces(sent_out(rows_out.astype(jnp.bfloat16)))
    cots_in = pieces(sent_out(cots_out.astype(jnp.bfloat16)))
    rows_full = [gather_cols(value, tp_own, tp_count) for value in rows_in]
    cots_full = [gather_cols(value, tp_own, tp_count) for value in cots_in]

    acts, gate_grads, up_grads, returned = [], [], [], []
    for routed_rows, routed_cots in zip(rows_full, cots_full):
        gate_pre = jnp.dot(routed_rows, w_gate, preferred_element_type=jnp.float32)
        up_pre = jnp.dot(routed_rows, w_up, preferred_element_type=jnp.float32)
        gate_clamped = jnp.minimum(gate_pre, CLAMP_LIMIT)
        up_clamped = jnp.clip(up_pre, -CLAMP_LIMIT, CLAMP_LIMIT)
        sigma = jax.nn.sigmoid(SLOPE_ALPHA * gate_clamped)
        gated = gate_clamped * sigma
        acts.append(((up_clamped + 1.0) * gated).astype(jnp.bfloat16))
        act_grad = contract_cols(routed_cots, w_down)
        inside = (up_pre > -CLAMP_LIMIT) & (up_pre < CLAMP_LIMIT)
        up_pre_grad = jnp.where(inside, act_grad * gated, 0.0).astype(jnp.bfloat16)
        slope = sigma + SLOPE_ALPHA * gate_clamped * sigma * (1.0 - sigma)
        gate_pre_grad = jnp.where(
            gate_pre < CLAMP_LIMIT, act_grad * (up_clamped + 1.0) * slope, 0.0
        ).astype(jnp.bfloat16)
        gate_grads.append(gate_pre_grad)
        up_grads.append(up_pre_grad)
        partial_value = contract_cols(gate_pre_grad, w_gate) + contract_cols(up_pre_grad, w_up)
        row_grad = scatter_cols(partial_value.astype(jnp.bfloat16), tp_own, tp_count)
        returned.append(sent_out(row_grad).reshape(-1, col_count))

    def weight_grad(lefts, rights):
        return sum(contract_rows(l, r) for l, r in zip(lefts, rights)).astype(jnp.bfloat16)

    down_grad = weight_grad(acts, cots_full)
    gate_grad = weight_grad(rows_full, gate_grads)
    up_grad = weight_grad(rows_full, up_grads)

    normed_part_grad = sum(
        contract_rows(
            chosen[:, chunk * piece : (chunk + 1) * piece].reshape(sp_count * piece, tok_rows),
            returned[chunk],
        )
        for chunk in range(send_chunks)
    ).astype(jnp.bfloat16)
    normed_grad = gather_cols(normed_part_grad, tp_own, tp_count)
    feature_grad = normed_grad.astype(jnp.float32) * norm_gain
    cubed = inv_rms * inv_rms * inv_rms
    resid_grad = (
        grad_out.astype(jnp.float32)
        + inv_rms * feature_grad
        - resid_f * cubed * jnp.mean(resid_f * feature_grad, axis=-1, keepdims=True)
    ).astype(jnp.bfloat16)
    channels = conv_sum.shape[1]
    summed = conv_sum.astype(jnp.float32).reshape(tok_rows, channels // GROUP, GROUP)
    centre = summed - jnp.mean(summed, axis=-1, keepdims=True)
    inv_std = lax.rsqrt(jnp.mean(centre * centre, axis=-1, keepdims=True) + 1e-05)
    grouped = centre * inv_std
    chan_normed = grouped.reshape(tok_rows, channels)
    pre_act = chan_normed * conv_gain
    sigma_conv = jax.nn.sigmoid(pre_act)
    conv_out = (pre_act * sigma_conv).astype(jnp.bfloat16)
    proj_term = contract_rows(resid_grad, conv_out).astype(jnp.bfloat16)
    terms = swapped(proj_term.reshape(sp_count, model_width // sp_count, channels))
    proj_grad = jnp.sum(terms.astype(jnp.float32), axis=0)
    out_grad = jnp.dot(resid_grad, proj_weight, preferred_element_type=jnp.float32)
    normal_grad = (
        out_grad * sigma_conv * (1.0 + pre_act * (1.0 - sigma_conv)) * conv_gain
    ).reshape(tok_rows, channels // GROUP, GROUP)
    sum_grad = inv_std * (
        normal_grad
        - jnp.mean(normal_grad, axis=-1, keepdims=True)
        - grouped * jnp.mean(normal_grad * grouped, axis=-1, keepdims=True)
    )
    sum_grad = sum_grad.reshape(tok_rows, channels)
    following = passed_along(sum_grad[: CONV_K - 1], "sp", -1)
    extended = jnp.concatenate([sum_grad, following], axis=0)
    gated_grad = lax.conv_general_dilated(
        extended[None],
        conv_taps[::-1][:, None, :],
        (1,),
        ((0, 0),),
        dimension_numbers=("NWC", "WIO", "NWC"),
        feature_group_count=channels,
        precision=lax.Precision.HIGHEST,
    )[0]
    sigma_gate = jax.nn.sigmoid(conv_gate.astype(jnp.float32))
    value_grad = (gated_grad * sigma_gate).astype(jnp.bfloat16)
    gate_input_grad = (
        gated_grad * conv_value.astype(jnp.float32) * sigma_gate * (1.0 - sigma_gate)
    ).astype(jnp.bfloat16)
    return (gate_grad[None], up_grad[None], down_grad[None], proj_grad, value_grad, gate_input_grad)


def solution(mesh):
    in_specs = (
        P("sp", None),
        P("sp", None),
        P(),
        P("sp", None),
        P("sp", None),
        P("sp", None, "tp"),
        P("sp", None, "tp"),
        P("sp", "tp", None),
        P(None, "tp"),
        P("sp", "tp"),
        P("tp"),
        P(None, "tp"),
        P("sp", "tp"),
        P("sp", "tp"),
    )
    out_specs = (
        P("sp", None, "tp"),
        P("sp", None, "tp"),
        P("sp", "tp", None),
        P("sp", "tp"),
        P("sp", "tp"),
        P("sp", "tp"),
    )
    return jax.shard_map(backward, mesh=mesh, in_specs=in_specs, out_specs=out_specs, check_vma=False)
```
